32 devices in a mesh: ep: 8 (over z, y), tp: 4 (over x, core).
Axes of the slice: x: 2, y: 2, z: 4, core: 2. Of those that a mesh axis runs over, the one named last changes fastest.
Arguments:
- gate_outer: bfloat16 [16384, 1024], P(('ep', 'tp')), may hold values from -6 to 6
- gate_inner: bfloat16 [16384, 1024], P(('ep', 'tp')), may hold values from -6 to 6
- conv_input: bfloat16 [16384, 1024], P(('ep', 'tp')), may hold values from -6 to 6
- conv_taps: float32 [3, 1024], replicated, may hold values from -3.5 to 3.5
- mixer_out_weight: bfloat16 [1024, 2048], replicated, may hold values from -0.1875 to 0.1875
- moe_tokens: bfloat16 [4096, 2048], P(('ep', 'tp')), may hold values from -40 to 40
- norm_gain: float32 [2048], replicated, may hold values from 0.1 to 1.9
- expert_ids: int32 [4096, 4], P(('ep', 'tp')), may hold values from 0 to 31, all different within a row; in each aligned block of 128 rows (0 to 127, 128 to 255, ...) at most 24 rows name the same one
- route_weight: float32 [4096, 4], P(('ep', 'tp')), may hold values from 0.2 to 1
- expert_gate: bfloat16 [32, 2048, 1024], P(('ep', 'tp')), may hold values from -0.39648438 to 0.39648438
- expert_up: bfloat16 [32, 2048, 1024], P(('ep', 'tp')), may hold values from -0.39648438 to 0.39648438
- expert_down: bfloat16 [32, 1024, 2048], P(('ep', 'tp')), may hold values from -0.03125 to 0.03125
Outputs:
- mixed_out: bfloat16 [16384, 2048], P(('ep', 'tp'))
- moe_out: bfloat16 [4096, 2048], P(('ep', 'tp'))
The draws below stay inside these ranges and needn't reach their ends.
Inputs may be any that keep to these rules, and one draw needn't show every extreme that they name: `expert_ids`: each token names 4 different experts. Among the tokens of one device no expert is named by more than 24 of them, and on some device an expert is named by exactly 24.
All inputs are finite; a program needn't handle non-finite values.
Results may differ from the reference program's by a relative error of at most 0.007.
Values may be sent and summed in bfloat16 or wider, within the bound.
No kernel may reach another device: no remote copies, remote signals or barrier semaphores. Data moves between devices by JAX's collectives and lax.ppermute only.
A program may use at most 128 MiB of HBM per device.

```python
import math
import jax
import jax.numpy as jnp
import numpy as np
from jax import lax

D = 2048
W_MIX = 1024
FF = 1024
TOP_K = 4
TAPS = 3
MOE_DEV = 128
EXPERTS = 32
CAP = 24
MIX_TOKENS = 16384
MOE_TOKENS = 4096
DEVICES = 32


def draw_moe_tokens(key, part):
    key_base = jax.random.fold_in(key, 101)
    key_scale = jax.random.fold_in(key, 202)
    base_values = jax.random.truncated_normal(key_base, -4.0, 4.0, (MOE_TOKENS, D), jnp.float32)
    row_scale = jnp.exp(jax.random.uniform(key_scale, (MOE_TOKENS, 1), jnp.float32, 0.0, math.log(10.0)))
    values = base_values * row_scale
    return values.astype(jnp.bfloat16)


def level_of(stream_key, extent, cuts, low, top_value):
    def one(axis_at, parts):
        heights = jax.random.uniform(jax.random.fold_in(jax.random.fold_in(stream_key, 6), axis_at), (parts,), jnp.float32, low / len(cuts), top_value / len(cuts))
        return jnp.repeat(jnp.exp(heights), extent[axis_at] // parts).reshape((-1,) + (1,) * (len(extent) - axis_at - 1))

    loudness = one(*cuts[0])
    for cut in cuts[1:]:
        loudness = loudness * one(*cut)
    return loudness


def shared_out(rng, own, number, rows, amount, top, reach, slope):
    ranking = jax.random.permutation(rng, amount)
    crowded, usual = shares(amount, rows * top, reach, slope, True), shares(amount, rows * top, reach, slope, False)
    places = jnp.arange(amount)

    def named(sizes, turn):
        used = int((sizes > 0).sum())
        fixed = max(1, used // 4)
        passed = fixed + (places - fixed + turn * (used - fixed)) % max(1, amount - fixed)
        return jnp.zeros((amount,), jnp.int32).at[ranking[jnp.where(places < fixed, places, passed)]].set(jnp.asarray(sizes, jnp.int32))

    sizes = jnp.where(number % 4 == 0, named(crowded, number // 4), named(usual, number - number // 4 - 1))
    mixed = jax.random.permutation(jax.random.fold_in(own, 3), amount)
    donor, receiver = mixed[0:amount // 2 * 2:2], mixed[1:amount // 2 * 2:2]
    room = jnp.minimum(sizes[donor] - 1, reach - sizes[receiver]) // 2
    room = jnp.where((donor == ranking[0]) | (receiver == ranking[0]) | (sizes[receiver] == 0), 0, jnp.maximum(room, 0))
    passed = jax.random.randint(jax.random.fold_in(own, 4), (amount // 2,), 0, 1 << 20) % (room + 1)
    sizes = sizes.at[donor].add(-passed).at[receiver].add(passed)
    labels = jnp.searchsorted(jnp.cumsum(sizes), jnp.arange(rows * top), side="right").astype(jnp.int32)
    listing = labels.reshape(top, rows).T
    listing = listing[jax.random.permutation(jax.random.fold_in(own, 1), rows)]
    turn = jax.random.randint(jax.random.fold_in(own, 2), (rows, 1), 0, top)
    return jnp.take_along_axis(listing, (jnp.arange(top)[None, :] + turn) % top, axis=1)


def shares(count, total, reach, skew, full):
    portions = [(1 << 20) // math.isqrt(grade ** skew) + 1 for grade in range(1, count + 1)]
    largest = reach if full else min(reach, max(-(-total // count), total * portions[0] // sum(portions)))
    least = 1 if total - largest >= count - 1 else 0
    given, spare = [largest] + [least] * (count - 1), total - largest - least * (count - 1)
    while spare > 0:
        free = [i for i in range(1, count) if given[i] < largest] or [i for i in range(1, count) if given[i] < reach]
        pool, left = sum([portions[i] for i in free]), spare
        for i in free:
            extra = min(reach - given[i], max(1, left * portions[i] // pool), spare)
            given[i] = given[i] + extra
            spare = spare - extra
    return np.array(given)


def scatter_about(key, shape, scale, most, cuts=(), kind=jnp.bfloat16):
    entries = jax.random.normal(key, shape, jnp.float32) * scale
    if len(cuts) > 0:
        entries = level_of(key, shape, cuts, -0.22, 0.18) * entries
    return jnp.clip(entries, min=-most, max=most).astype(kind)


def setup_inputs(seed: int = 0) -> dict:
    splits = jax.random.split(jax.random.key(seed), 13)
    gate_outer = scatter_about(splits[0], (MIX_TOKENS, W_MIX), 1.0, 6.0, ((0, 32),))
    gate_inner = scatter_about(splits[1], (MIX_TOKENS, W_MIX), 1.0, 6.0, ((0, 32),))
    conv_input = scatter_about(splits[2], (MIX_TOKENS, W_MIX), 1.0, 6.0, ((0, 32),))
    conv_taps = scatter_about(splits[3], (TAPS, W_MIX), TAPS ** -0.5, 3.5, (), jnp.float32)
    mixer_out_weight = scatter_about(splits[4], (W_MIX, D), W_MIX ** -0.5, 0.1875)
    moe_tokens = draw_moe_tokens(jax.random.fold_in(splits[12], 71), 0)
    norm_gain = jnp.clip(1.0 + 0.18 * jax.random.normal(splits[6], (D,), jnp.float32), 0.1, 1.9)
    expert_ids_keys = jax.random.split(jax.random.fold_in(splits[7], 1), MOE_TOKENS // MOE_DEV)
    expert_ids_turns = jax.random.permutation(jax.random.fold_in(splits[7], 3), MOE_TOKENS // MOE_DEV)
    expert_ids = jax.vmap(lambda own, number: shared_out(jax.random.fold_in(splits[7], 2), own, number, MOE_DEV, EXPERTS, TOP_K, CAP, 2))(expert_ids_keys, expert_ids_turns).reshape((MOE_TOKENS, TOP_K))
    route_weight = jnp.clip(jnp.exp(math.log(1.0) - 1.609438 * jax.random.uniform(splits[8], (MOE_TOKENS, TOP_K), jnp.float32) ** level_of(splits[8], (MOE_TOKENS, TOP_K), ((0, 32),), -0.2, 0.2)), 0.2, 1.0)
    expert_gate = scatter_about(splits[9], (EXPERTS, D, FF), (3.0 * D ** -0.5), 0.39648438, ((0, 32),))
    expert_up = scatter_about(splits[10], (EXPERTS, D, FF), (3.0 * D ** -0.5), 0.39648438, ((0, 32),))
    expert_down = scatter_about(splits[11], (EXPERTS, FF, D), (FF ** -0.5 / 6.0), 0.03125, ((0, 32),))
    return {"gate_outer": gate_outer, "gate_inner": gate_inner, "conv_input": conv_input, "conv_taps": conv_taps, "mixer_out_weight": mixer_out_weight, "moe_tokens": moe_tokens, "norm_gain": norm_gain, "expert_ids": expert_ids, "route_weight": route_weight, "expert_gate": expert_gate, "expert_up": expert_up, "expert_down": expert_down}


epsilon = 1e-06
clamp_limit = 7.0
alpha_gate = 1.702

def expert_rows(row_block, gate_weight, up_weight, down_weight):
    gate_pre = jnp.dot(row_block, gate_weight, preferred_element_type=jnp.float32)
    up_pre = jnp.dot(row_block, up_weight, preferred_element_type=jnp.float32)
    gate_pre = jnp.minimum(gate_pre, clamp_limit)
    up_pre = jnp.clip(up_pre, -clamp_limit, clamp_limit)
    hidden = ((up_pre + 1.0) * (gate_pre * jax.nn.sigmoid(alpha_gate * gate_pre))).astype(jnp.bfloat16)
    return jnp.dot(hidden, down_weight, preferred_element_type=jnp.float32).astype(jnp.bfloat16)

def reference(gate_outer, gate_inner, conv_input, conv_taps, mixer_out_weight, moe_tokens, norm_gain, expert_ids, route_weight, expert_gate, expert_up, expert_down):
    product = (gate_inner.astype(jnp.float32) * conv_input.astype(jnp.float32)).astype(jnp.bfloat16)
    padded = jnp.concatenate([jnp.zeros((TAPS - 1, W_MIX), jnp.float32), product.astype(jnp.float32)], 0)
    convolved = jnp.zeros((MIX_TOKENS, W_MIX), jnp.float32)
    for offset in range(TAPS):
        convolved = convolved + conv_taps[offset][None, :] * padded[offset:offset + MIX_TOKENS]
    gated = (gate_outer.astype(jnp.float32) * convolved).astype(jnp.bfloat16)
    mixed_out = jnp.dot(gated, mixer_out_weight, preferred_element_type=jnp.float32).astype(jnp.bfloat16)
    widened = moe_tokens.astype(jnp.float32)
    normed = (widened * lax.rsqrt(lax.optimization_barrier(jnp.mean(widened * widened, axis=-1, keepdims=True)) + epsilon) * norm_gain.astype(jnp.float32)).astype(jnp.bfloat16)
    mix_weight = route_weight / lax.optimization_barrier(jnp.sum(route_weight, axis=-1, keepdims=True))
    flat_ids = expert_ids.reshape(-1).astype(jnp.int32)
    copy_weight = mix_weight.reshape(-1)
    copy_order = jnp.argsort(flat_ids, stable=True).astype(jnp.int32)
    counts = jax.ops.segment_sum(jnp.ones_like(flat_ids), flat_ids, EXPERTS).astype(jnp.int32)
    starts = (jnp.cumsum(counts) - counts).astype(jnp.int32)
    row_limit = DEVICES * CAP
    order_padded = jnp.concatenate([copy_order, jnp.zeros((row_limit,), jnp.int32)], 0)
    positions = jnp.arange(row_limit, dtype=jnp.int32)

    def per_expert(totals, expert):
        picked = lax.dynamic_slice_in_dim(order_padded, starts[expert].astype(jnp.int32), row_limit)
        is_valid = positions < counts[expert]
        token_index = (picked // TOP_K).astype(jnp.int32)
        row_block = normed[token_index]
        expert_out = expert_rows(row_block, expert_gate[expert], expert_up[expert], expert_down[expert])
        scaled = jnp.where(is_valid, copy_weight[picked], jnp.zeros_like(copy_weight[picked]))
        totals = totals.at[token_index].add(scaled[:, None] * expert_out.astype(jnp.float32))
        return (totals, None)
    totals, _ = lax.scan(per_expert, jnp.zeros((MOE_TOKENS, D), jnp.float32), jnp.arange(EXPERTS, dtype=jnp.int32))
    moe_out = totals.astype(jnp.bfloat16)
    return (mixed_out, moe_out)
```

```python
import jax
import jax.numpy as jnp
from jax import lax
from jax.sharding import Mesh, PartitionSpec as P

epsilon = 1e-06
clamp_limit = 7.0
alpha_gate = 1.702
EVERY = ("half", "near", "tp")
NEAR = ("near", "tp")


def from_behind(value, axis, by):
    length = lax.axis_size(axis)
    pairs = [(i, i + by) for i in range(length) if 0 <= i + by < length]
    return lax.ppermute(value, axis, pairs)


def swap_halves(value):
    length = lax.axis_size("half")
    return lax.ppermute(value, "half", [(i, (i + 1) % length) for i in range(length)])


def expert_rows(row_block, gate_weight, up_weight, down_weight):
    gate_pre = jnp.dot(row_block, gate_weight, preferred_element_type=jnp.float32)
    up_pre = jnp.dot(row_block, up_weight, preferred_element_type=jnp.float32)
    gate_pre = jnp.minimum(gate_pre, clamp_limit)
    up_pre = jnp.clip(up_pre, -clamp_limit, clamp_limit)
    hidden = ((up_pre + 1.0) * (gate_pre * jax.nn.sigmoid(alpha_gate * gate_pre))).astype(
        jnp.bfloat16
    )
    return jnp.dot(hidden, down_weight, preferred_element_type=jnp.float32).astype(jnp.bfloat16)


def norm_rows(tokens, norm_gain):
    widened = tokens.astype(jnp.float32)
    return (
        widened
        * lax.rsqrt(jnp.mean(widened * widened, axis=-1, keepdims=True) + epsilon)
        * norm_gain[None, :]
    ).astype(jnp.bfloat16)


def slot_maps(routing, first_expert, experts_near, capacity):
    top_count = routing.shape[0] // 2
    tokens = routing.shape[1]
    ids = routing[:top_count].astype(jnp.int32)
    weights = routing[top_count:]
    mix_weight = weights / jnp.sum(weights, axis=0, keepdims=True)
    experts = first_expert + lax.broadcasted_iota(jnp.int32, (experts_near, 1), 0)
    named = jnp.zeros((experts_near, tokens), jnp.float32)
    share = jnp.zeros((experts_near, tokens), jnp.float32)
    for choice in range(top_count):
        hit = ids[choice][None, :] == experts
        named = named + hit.astype(jnp.float32)
        share = share + jnp.where(hit, mix_weight[choice][None, :], 0.0)
    before = lax.broadcasted_iota(jnp.int32, (tokens, tokens), 0) < lax.broadcasted_iota(
        jnp.int32, (tokens, tokens), 1
    )
    rank = jnp.dot(
        named.astype(jnp.bfloat16), before.astype(jnp.bfloat16), preferred_element_type=jnp.float32
    )
    slots = lax.broadcasted_iota(jnp.int32, (experts_near, capacity, tokens), 1)
    rank = jnp.where(named > 0, rank.astype(jnp.int32), capacity)
    here = rank[:, None, :] == slots
    dispatch = here.astype(jnp.bfloat16).reshape(experts_near * capacity, tokens)
    combine = jnp.where(here, share[:, None, :], 0.0).reshape(experts_near * capacity, tokens)
    return dispatch, combine


def to_experts(dispatch, rows, members):
    send = jnp.dot(dispatch, rows, preferred_element_type=jnp.float32).astype(jnp.bfloat16)
    send = send.reshape(members, -1, rows.shape[1])
    return lax.all_to_all(send, NEAR, split_axis=0, concat_axis=0, tiled=True)


def from_experts(combine, rows, received_shape):
    back = lax.all_to_all(
        rows.reshape(received_shape), NEAR, split_axis=0, concat_axis=0, tiled=True
    ).reshape(rows.shape)
    high = lax.reduce_precision(combine, 8, 7)
    low = combine - high
    total = None
    for part in (high, low):
        term = lax.dot_general(
            part.astype(jnp.bfloat16),
            back,
            (((0,), (0,)), ((), ())),
            preferred_element_type=jnp.float32,
        )
        total = term if total is None else total + term
    return total


def shards(
    gate_outer,
    gate_inner,
    conv_input,
    conv_taps,
    mixer_out_weight,
    moe_tokens,
    norm_gain,
    expert_ids,
    route_weight,
    expert_gate,
    expert_up,
    expert_down,
):
    tokens_here, width = moe_tokens.shape
    top_count = expert_ids.shape[1]
    experts_near = lax.axis_size(NEAR)
    experts_all = lax.axis_size(EVERY)
    capacity = 3 * tokens_here * top_count // (2 * experts_all)
    first_expert = lax.axis_index("half") * experts_near

    routing = jnp.concatenate([expert_ids.T.astype(jnp.float32), route_weight.T], 0)
    far_routing = swap_halves(routing)
    far_tokens = swap_halves(moe_tokens)

    dispatch, combine = slot_maps(routing, first_expert, experts_near, capacity)
    received = to_experts(dispatch, norm_rows(moe_tokens, norm_gain), experts_near)

    reach_rows = conv_taps.shape[0] - 1
    rows_here = gate_inner.shape[0]
    product = (gate_inner.astype(jnp.float32) * conv_input.astype(jnp.float32)).astype(jnp.bfloat16)
    previous = from_behind(product[rows_here - reach_rows :], EVERY, 1)
    extended = jnp.concatenate([previous, product], 0).astype(jnp.float32)
    convolved = jnp.zeros(product.shape, jnp.float32)
    for offset in range(conv_taps.shape[0]):
        convolved = convolved + conv_taps[offset][None, :] * extended[offset : offset + rows_here]
    gated_rows = (gate_outer.astype(jnp.float32) * convolved).astype(jnp.bfloat16)
    mixed_out = jnp.dot(
        gated_rows, mixer_out_weight, preferred_element_type=jnp.float32
    ).astype(jnp.bfloat16)

    far_dispatch, far_combine = slot_maps(far_routing, first_expert, experts_near, capacity)
    far_received = to_experts(far_dispatch, norm_rows(far_tokens, norm_gain), experts_near)

    expert_out = expert_rows(
        received.reshape(-1, width), expert_gate[0], expert_up[0], expert_down[0]
    )
    far_out = expert_rows(
        far_received.reshape(-1, width), expert_gate[0], expert_up[0], expert_down[0]
    )
    far_total = from_experts(far_combine, far_out, received.shape).astype(jnp.bfloat16)
    returned = swap_halves(far_total)
    total = from_experts(combine, expert_out, received.shape)
    moe_out = (total + returned.astype(jnp.float32)).astype(jnp.bfloat16)
    return (mixed_out, moe_out)


def solution(mesh):
    outer, inner = mesh.shape["ep"], mesh.shape["tp"]
    halves = 2 if outer % 2 == 0 else 1
    split = Mesh(mesh.devices.reshape(halves, outer // halves, inner), EVERY)
    rows = P(EVERY, None)
    weights = P(EVERY, None, None)
    in_specs = (rows, rows, rows, P(), P(), rows, P(), rows, rows, weights, weights, weights)
    return jax.shard_map(
        shards, mesh=split, in_specs=in_specs, out_specs=(rows, rows), check_vma=False
    )
```

```python
import functools
import math

import jax
import jax.numpy as jnp
from jax import lax
from jax.experimental import pallas as pl
from jax.experimental.pallas import tpu as pltpu
from jax.sharding import Mesh, PartitionSpec as P

epsilon = 1e-06
clamp_limit = 7.0
alpha_gate = 1.702
EVERY = ("half", "near", "tp")
NEAR = ("near", "tp")
SMALL_VMEM = 12 * 1024 * 1024
WIDE_VMEM = 58 * 1024 * 1024
AHEAD = 3


def from_behind(value, axis, by):
    length = lax.axis_size(axis)
    pairs = [(i, i + by) for i in range(length) if 0 <= i + by < length]
    return lax.ppermute(value, axis, pairs)


def swap_halves(value):
    halves, near = lax.axis_size("half"), lax.axis_size("near")
    shift = near // 2 if near % 2 == 0 and halves > 1 else 0
    pairs = [
        (h * near + n, (h + 1) % halves * near + (n + shift) % near)
        for h in range(halves)
        for n in range(near)
    ]
    return lax.ppermute(value, ("half", "near"), pairs)


def dispatch_kernel(
    capacity, masked, place_ref, ids_ref, weight_ref, rows_ref, gain_ref, slot_ref, mix_ref, *send_refs
):
    top_count, tokens = ids_ref.shape
    slots = sum(ref.shape[0] for ref in send_refs)
    experts_near = slots // capacity
    ids = ids_ref[...] - place_ref[0]
    weights = weight_ref[...]
    mix_ref[...] = weights / jnp.sum(weights, axis=0, keepdims=True)
    experts = lax.broadcasted_iota(jnp.int32, (experts_near, tokens), 0)
    hits = [ids[k : k + 1, :] == experts for k in range(top_count)]
    named = functools.reduce(jnp.logical_or, hits)
    before = lax.broadcasted_iota(jnp.int32, (tokens, tokens), 0) < lax.broadcasted_iota(
        jnp.int32, (tokens, tokens), 1
    )
    rank = jnp.dot(
        named.astype(jnp.float32).astype(jnp.bfloat16),
        before.astype(jnp.float32).astype(jnp.bfloat16),
        preferred_element_type=jnp.float32,
    )
    slot_rows = lax.broadcasted_iota(jnp.int32, (slots, tokens), 0)
    here = None
    for k in range(top_count):
        own = jnp.sum(jnp.where(hits[k], rank, 0.0), axis=0, keepdims=True).astype(jnp.int32)
        choice = ids[k : k + 1, :]
        inside = (choice >= 0) & (choice < experts_near)
        block = choice ^ place_ref[1] if masked else choice
        slot = jnp.where(inside, block * capacity + own, slots)
        slot_ref[k : k + 1, :] = slot
        match = slot_rows == slot
        here = match if here is None else here | match
    widened = rows_ref[...].astype(jnp.float32)
    normed = (
        widened
        * lax.rsqrt(jnp.mean(widened * widened, axis=-1, keepdims=True) + epsilon)
        * gain_ref[...]
    ).astype(jnp.bfloat16)
    laid = jnp.dot(
        here.astype(jnp.float32).astype(jnp.bfloat16), normed, preferred_element_type=jnp.float32
    )
    start = 0
    for ref in send_refs:
        ref[...] = laid[start : start + ref.shape[0]].astype(ref.dtype)
        start += ref.shape[0]


def block_shapes(slots, width, blocks):
    return [jax.ShapeDtypeStruct((slots // blocks, width), jnp.bfloat16)] * blocks


def to_slots(place, ids, weights, rows, gain, slots, capacity, blocks, room):
    top_count, tokens = ids.shape
    width = rows.shape[1]
    held = pl.BlockSpec(memory_space=pltpu.VMEM)
    slot, mix, *send = pl.pallas_call(
        functools.partial(dispatch_kernel, capacity, blocks > 1),
        in_specs=[pl.BlockSpec(memory_space=pltpu.SMEM)] + [held] * 4,
        out_specs=[held] * (2 + blocks),
        out_shape=[
            jax.ShapeDtypeStruct((top_count, tokens), jnp.int32),
            jax.ShapeDtypeStruct((top_count, tokens), jnp.float32),
        ]
        + block_shapes(slots, width, blocks),
        compiler_params=pltpu.CompilerParams(vmem_limit_bytes=room),
        cost_estimate=pl.CostEstimate(
            flops=2 * slots * tokens * width,
            bytes_accessed=2 * (slots + tokens) * width,
            transcendentals=tokens,
        ),
    )(place, ids, weights, rows, gain)
    return slot, mix, send


def gather_blocks(refs, wide_ref):
    if len(refs) == 1:
        return refs[0][...]
    start = 0
    for ref in refs:
        wide_ref[start : start + ref.shape[0], :] = ref[...].astype(jnp.float32)
        start += ref.shape[0]
    return wide_ref[...].astype(jnp.bfloat16)


def combine_kernel(blocks, addends, slot_ref, mix_ref, *refs):
    back_refs, add_refs = refs[:blocks], refs[blocks : blocks + addends]
    out_ref, wide_ref = refs[blocks + addends :]
    slots = sum(ref.shape[0] for ref in back_refs)
    top_count, tokens = slot_ref.shape
    slot_rows = lax.broadcasted_iota(jnp.int32, (slots, tokens), 0)
    share = jnp.zeros((slots, tokens), jnp.float32)
    for k in range(top_count):
        share = jnp.where(slot_rows == slot_ref[k : k + 1, :], mix_ref[k : k + 1, :], share)
    high = share.astype(jnp.bfloat16)
    low = (share - high.astype(jnp.float32)).astype(jnp.bfloat16)
    back = gather_blocks(back_refs, wide_ref)
    over = (((0,), (0,)), ((), ()))
    total = lax.dot_general(high, back, over, preferred_element_type=jnp.float32)
    total = total + lax.dot_general(low, back, over, preferred_element_type=jnp.float32)
    for ref in add_refs:
        total = total + ref[...].astype(jnp.float32)
    out_ref[...] = total.astype(out_ref.dtype)


def from_slots(slot, mix, back, addends):
    slots, width = sum(block.shape[0] for block in back), back[0].shape[1]
    tokens = slot.shape[1]
    wide = (slots, width) if len(back) > 1 else (8, 128)
    return pl.pallas_call(
        functools.partial(combine_kernel, len(back), len(addends)),
        in_specs=[pl.BlockSpec(memory_space=pltpu.VMEM)] * (2 + len(back) + len(addends)),
        out_specs=pl.BlockSpec(memory_space=pltpu.VMEM),
        out_shape=jax.ShapeDtypeStruct((tokens, width), jnp.bfloat16),
        scratch_shapes=[pltpu.VMEM(wide, jnp.float32)],
        compiler_params=pltpu.CompilerParams(vmem_limit_bytes=SMALL_VMEM),
        cost_estimate=pl.CostEstimate(
            flops=4 * slots * tokens * width,
            bytes_accessed=2 * (slots + tokens) * width,
            transcendentals=0,
        ),
    )(slot, mix, *back, *addends)


def expert_kernel(blocks, gate, up, down, *refs):
    in_refs, out_refs = refs[:blocks], refs[blocks : 2 * blocks]
    gate_ref, up_ref, down_ref, hidden_ref, wide_ref, sems = refs[2 * blocks :]
    parts, _, tile = gate_ref.shape
    columns, _, column = down_ref.shape
    work = []
    for part in range(parts):
        cut = pl.ds(part * tile, tile)
        work.append(((gate, gate_ref, part, cut), (up, up_ref, part, cut)))
    for part in range(columns):
        work.append(((down, down_ref, part, pl.ds(part * column, column)),))
    copies = [
        [
            pltpu.make_async_copy(source.at[0, :, cut], target.at[part], sems.at[step, at])
            for at, (source, target, part, cut) in enumerate(pieces)
        ]
        for step, pieces in enumerate(work)
    ]

    def ready(step):
        for copy in copies[step]:
            copy.wait()
        if step + AHEAD < len(copies):
            for copy in copies[step + AHEAD]:
                copy.start()

    for step in range(min(AHEAD, len(copies))):
        for copy in copies[step]:
            copy.start()
    rows = gather_blocks(in_refs, wide_ref)
    for part in range(parts):
        ready(part)
        gate_pre = jnp.dot(rows, gate_ref[part], preferred_element_type=jnp.float32)
        up_pre = jnp.dot(rows, up_ref[part], preferred_element_type=jnp.float32)
        gate_pre = jnp.minimum(gate_pre, clamp_limit)
        up_pre = jnp.clip(up_pre, -clamp_limit, clamp_limit)
        hidden_ref[:, part * tile : (part + 1) * tile] = (
            (up_pre + 1.0) * (gate_pre * jax.nn.sigmoid(alpha_gate * gate_pre))
        ).astype(jnp.bfloat16)
    for part in range(columns):
        ready(parts + part)
        result = jnp.dot(hidden_ref[...], down_ref[part], preferred_element_type=jnp.float32)
        start = 0
        for ref in out_refs:
            ref[:, part * column : (part + 1) * column] = result[
                start : start + ref.shape[0]
            ].astype(ref.dtype)
            start += ref.shape[0]


def expert_rows(rows, weights):
    count, width = sum(block.shape[0] for block in rows), rows[0].shape[1]
    hidden = weights[0].shape[2]
    tile, column = math.gcd(hidden, 256), math.gcd(width, 512)
    parts, columns = hidden // tile, width // column
    held = pl.BlockSpec(memory_space=pltpu.VMEM)
    wide = (count, width) if len(rows) > 1 else (8, 128)
    return pl.pallas_call(
        functools.partial(expert_kernel, len(rows)),
        in_specs=[pl.BlockSpec(memory_space=pl.ANY)] * 3 + [held] * len(rows),
        out_specs=[held] * len(rows),
        out_shape=block_shapes(count, width, len(rows)),
        scratch_shapes=[
            pltpu.VMEM((parts, width, tile), jnp.bfloat16),
            pltpu.VMEM((parts, width, tile), jnp.bfloat16),
            pltpu.VMEM((columns, hidden, column), jnp.bfloat16),
            pltpu.VMEM((count, hidden), jnp.bfloat16),
            pltpu.VMEM(wide, jnp.float32),
            pltpu.SemaphoreType.DMA((parts + columns, 2)),
        ],
        compiler_params=pltpu.CompilerParams(vmem_limit_bytes=WIDE_VMEM),
        cost_estimate=pl.CostEstimate(
            flops=6 * count * width * hidden,
            bytes_accessed=2 * (3 * width * hidden + 2 * count * width),
            transcendentals=count * hidden,
        ),
    )(*weights, *rows)


def hop_order(members):
    ranked = sorted(range(2, members), key=lambda mask: bin(mask >> 1).count("1"))
    mixed = []
    while ranked:
        mixed.append(ranked.pop())
        if ranked:
            mixed.append(ranked.pop(0))
    return mixed + [1] * (members > 1)


def hops(blocks, masks):
    members = len(blocks)
    arrived = {
        mask: lax.ppermute(blocks[mask], NEAR, [(i, i ^ mask) for i in range(members)])
        for mask in masks
    }
    return arrived


def in_order(first, arrived):
    return [first] + [arrived[mask] for mask in sorted(arrived)]


def exchange(rows, members):
    parts = rows.reshape(members, -1, rows.shape[1])
    return lax.all_to_all(parts, NEAR, split_axis=0, concat_axis=0, tiled=True).reshape(rows.shape)


def gated_input(gate_inner, conv_input):
    return (gate_inner.astype(jnp.float32) * conv_input.astype(jnp.float32)).astype(jnp.bfloat16)


def mixer(gate_outer, gate_inner, conv_input, previous, conv_taps, mixer_out_weight):
    rows_here = gate_inner.shape[0]
    product = gated_input(gate_inner, conv_input)
    extended = jnp.concatenate([previous, product], 0).astype(jnp.float32)
    convolved = jnp.zeros(product.shape, jnp.float32)
    for offset in range(conv_taps.shape[0]):
        convolved = convolved + conv_taps[offset][None, :] * extended[offset : offset + rows_here]
    gated_rows = (gate_outer.astype(jnp.float32) * convolved).astype(jnp.bfloat16)
    return jnp.dot(gated_rows, mixer_out_weight, preferred_element_type=jnp.float32).astype(
        jnp.bfloat16
    )


def shards(
    gate_outer,
    gate_inner,
    conv_input,
    conv_taps,
    mixer_out_weight,
    moe_tokens,
    norm_gain,
    expert_ids,
    route_weight,
    expert_gate,
    expert_up,
    expert_down,
):
    tokens_here, top_count = expert_ids.shape
    members = lax.axis_size(NEAR)
    capacity = 3 * tokens_here * top_count // (2 * lax.axis_size(EVERY))
    capacity = -(-capacity // 8) * 8
    slots = members * capacity
    masks = hop_order(members)
    place = jnp.stack([lax.axis_index("half") * members, lax.axis_index(NEAR)])
    gain = norm_gain[None, :]
    ids, route = expert_ids.T, route_weight.T
    weights = (expert_gate, expert_up, expert_down)

    far_tokens = swap_halves(moe_tokens)
    far_ids = swap_halves(ids)
    far_route = swap_halves(route)
    last = gate_inner.shape[0] - (conv_taps.shape[0] - 1)
    previous = from_behind(gated_input(gate_inner[last:], conv_input[last:]), EVERY, 1)
    slot, mix, send = to_slots(
        place, ids, route, moe_tokens, gain, slots, capacity, members, WIDE_VMEM
    )
    far_slot, far_mix, far_send = to_slots(
        place, far_ids, far_route, far_tokens, gain, slots, capacity, 1, SMALL_VMEM
    )
    far_received = exchange(far_send[0], members)
    received = in_order(send[0], hops(send, masks))
    far_out = expert_rows([far_received], weights)
    far_back = exchange(far_out[0], members)
    out = expert_rows(received, weights)
    back = hops(out, masks[: members // 2])
    far_total = from_slots(far_slot, far_mix, [far_back], ())
    returned = swap_halves(far_total)
    back |= hops(out, masks[members // 2 :])
    mixed_out = mixer(
        gate_outer, gate_inner, conv_input, previous, conv_taps, mixer_out_weight
    )
    back = in_order(out[0], back)
    moe_out = from_slots(slot, mix, back, (returned,))
    return (mixed_out, moe_out)


def solution(mesh):
    outer, inner = mesh.shape["ep"], mesh.shape["tp"]
    halves = 2 if outer % 2 == 0 else 1
    split = Mesh(mesh.devices.reshape(halves, outer // halves, inner), EVERY)
    rows = P(EVERY, None)
    weights = P(EVERY, None, None)
    in_specs = (rows, rows, rows, P(), P(), rows, P(), rows, rows, weights, weights, weights)
    return jax.shard_map(
        shards, mesh=split, in_specs=in_specs, out_specs=(rows, rows), check_vma=False
    )
```

```python
import functools
import math

import jax
import jax.numpy as jnp
from jax import lax
from jax.experimental import pallas as pl
from jax.experimental.pallas import tpu as pltpu
from jax.sharding import Mesh, PartitionSpec as P

epsilon = 1e-06
clamp_limit = 7.0
alpha_gate = 1.702
EVERY = ("half", "near", "tp")
NEAR = ("near", "tp")
SMALL_VMEM = 12 * 1024 * 1024
WIDE_VMEM = 58 * 1024 * 1024
EXPERT_VMEM = 50 * 1024 * 1024
AHEAD = 5


def from_behind(value, axis, by):
    length = lax.axis_size(axis)
    pairs = [(i, i + by) for i in range(length) if 0 <= i + by < length]
    return lax.ppermute(value, axis, pairs)


def swap_halves(value):
    halves, near = lax.axis_size("half"), lax.axis_size("near")
    shift = near // 2 if near % 2 == 0 and halves > 1 else 0
    pairs = [
        (h * near + n, (h + 1) % halves * near + (n + shift) % near)
        for h in range(halves)
        for n in range(near)
    ]
    return lax.ppermute(value, ("half", "near"), pairs)


def dispatch_kernel(capacity, masked, ids_ref, rows_ref, slot_ref, *send_refs):
    top_count, tokens = ids_ref.shape
    slots = sum(ref.shape[0] for ref in send_refs)
    experts_near = slots // capacity
    ids = ids_ref[...] - lax.axis_index("half") * experts_near
    member = lax.axis_index("near") * lax.axis_size("tp") + lax.axis_index("tp")
    experts = lax.broadcasted_iota(jnp.int32, (experts_near, tokens), 0)
    hits = [ids[k : k + 1, :] == experts for k in range(top_count)]
    named = functools.reduce(jnp.logical_or, hits)
    before = lax.broadcasted_iota(jnp.int32, (tokens, tokens), 0) < lax.broadcasted_iota(
        jnp.int32, (tokens, tokens), 1
    )
    rank = jnp.dot(
        named.astype(jnp.float32).astype(jnp.bfloat16),
        before.astype(jnp.float32).astype(jnp.bfloat16),
        preferred_element_type=jnp.float32,
    )
    slot_rows = lax.broadcasted_iota(jnp.int32, (slots, tokens), 0)
    here = None
    for k in range(top_count):
        own = jnp.sum(jnp.where(hits[k], rank, 0.0), axis=0, keepdims=True).astype(jnp.int32)
        choice = ids[k : k + 1, :]
        inside = (choice >= 0) & (choice < experts_near)
        block = choice ^ member if masked else choice
        slot = jnp.where(inside, block * capacity + own, slots)
        slot_ref[k : k + 1, :] = slot
        match = slot_rows == slot
        here = match if here is None else here | match
    laid = jnp.dot(
        here.astype(jnp.float32).astype(jnp.bfloat16),
        rows_ref[...],
        preferred_element_type=jnp.float32,
    )
    start = 0
    for ref in send_refs:
        ref[...] = laid[start : start + ref.shape[0]].astype(ref.dtype)
        start += ref.shape[0]


def block_shapes(slots, width, blocks):
    return [jax.ShapeDtypeStruct((slots // blocks, width), jnp.bfloat16)] * blocks


def to_slots(ids, rows, slots, capacity, blocks, room):
    top_count, tokens = ids.shape
    width = rows.shape[1]
    held = pl.BlockSpec(memory_space=pltpu.VMEM)
    slot, *send = pl.pallas_call(
        functools.partial(dispatch_kernel, capacity, blocks > 1),
        in_specs=[held, held],
        out_specs=[held] * (1 + blocks),
        out_shape=[jax.ShapeDtypeStruct((top_count, tokens), jnp.int32)]
        + block_shapes(slots, width, blocks),
        compiler_params=pltpu.CompilerParams(vmem_limit_bytes=room),
        cost_estimate=pl.CostEstimate(
            flops=2 * slots * tokens * width,
            bytes_accessed=2 * (slots + tokens) * width,
            transcendentals=0,
        ),
    )(ids, rows)
    return slot, send


def gather_blocks(refs, wide_ref):
    if len(refs) == 1:
        return refs[0][...]
    start = 0
    for ref in refs:
        wide_ref[start : start + ref.shape[0], :] = ref[...].astype(jnp.float32)
        start += ref.shape[0]
    return wide_ref[...].astype(jnp.bfloat16)


def combine_kernel(blocks, addends, slot_ref, weight_ref, *refs):
    back_refs, add_refs = refs[:blocks], refs[blocks : blocks + addends]
    out_ref, wide_ref = refs[blocks + addends :]
    slots = sum(ref.shape[0] for ref in back_refs)
    top_count, tokens = slot_ref.shape
    weights = weight_ref[...]
    mix = weights / jnp.sum(weights, axis=0, keepdims=True)
    slot_rows = lax.broadcasted_iota(jnp.int32, (slots, tokens), 0)
    share = jnp.zeros((slots, tokens), jnp.float32)
    for k in range(top_count):
        share = jnp.where(slot_rows == slot_ref[k : k + 1, :], mix[k : k + 1, :], share)
    high = share.astype(jnp.bfloat16)
    low = (share - high.astype(jnp.float32)).astype(jnp.bfloat16)
    back = gather_blocks(back_refs, wide_ref)
    over = (((0,), (0,)), ((), ()))
    total = lax.dot_general(high, back, over, preferred_element_type=jnp.float32)
    total = total + lax.dot_general(low, back, over, preferred_element_type=jnp.float32)
    for ref in add_refs:
        total = total + ref[...].astype(jnp.float32)
    out_ref[...] = total.astype(out_ref.dtype)


def from_slots(slot, weights, back, addends):
    slots, width = sum(block.shape[0] for block in back), back[0].shape[1]
    tokens = slot.shape[1]
    wide = (slots, width) if len(back) > 1 else (8, 128)
    return pl.pallas_call(
        functools.partial(combine_kernel, len(back), len(addends)),
        in_specs=[pl.BlockSpec(memory_space=pltpu.VMEM)] * (2 + len(back) + len(addends)),
        out_specs=pl.BlockSpec(memory_space=pltpu.VMEM),
        out_shape=jax.ShapeDtypeStruct((tokens, width), jnp.bfloat16),
        scratch_shapes=[pltpu.VMEM(wide, jnp.float32)],
        compiler_params=pltpu.CompilerParams(vmem_limit_bytes=SMALL_VMEM),
        cost_estimate=pl.CostEstimate(
            flops=4 * slots * tokens * width,
            bytes_accessed=2 * (slots + tokens) * width,
            transcendentals=0,
        ),
    )(slot, weights, *back, *addends)


def expert_kernel(blocks, gain, gate, up, down, *refs):
    in_refs, out_refs = refs[:blocks], refs[blocks : 2 * blocks]
    gate_ref, up_ref, down_ref, hidden_ref, wide_ref, rows_ref, gain_ref, sems = refs[2 * blocks :]
    parts, _, tile = gate_ref.shape
    columns, _, column = down_ref.shape
    work = []
    for part in range(parts):
        cut = pl.ds(part * tile, tile)
        work.append(((gate, gate_ref, part, cut), (up, up_ref, part, cut)))
    for part in range(columns):
        work.append(((down, down_ref, part, pl.ds(part * column, column)),))
    copies = [
        [
            pltpu.make_async_copy(source.at[0, :, cut], target.at[part], sems.at[step, at])
            for at, (source, target, part, cut) in enumerate(pieces)
        ]
        for step, pieces in enumerate(work)
    ]

    def ready(step):
        for copy in copies[step]:
            copy.wait()
        if step + AHEAD < len(copies):
            for copy in copies[step + AHEAD]:
                copy.start()

    scale_copy = pltpu.make_async_copy(gain, gain_ref, sems.at[len(copies), 0])
    scale_copy.start()
    for step in range(min(AHEAD, len(copies))):
        for copy in copies[step]:
            copy.start()
    height = in_refs[0].shape[0]
    for block, ref in enumerate(in_refs):
        wide_ref[block * height : (block + 1) * height, :] = ref[...].astype(jnp.float32)
    scale_copy.wait()
    count = wide_ref.shape[0]
    band = math.gcd(count, 64)
    for top in range(0, count, band):
        tokens = wide_ref[top : top + band, :]
        scale = lax.rsqrt(jnp.mean(tokens * tokens, axis=-1, keepdims=True) + epsilon)
        rows_ref[top : top + band, :] = (tokens * scale * gain_ref[...]).astype(jnp.bfloat16)
    for part in range(parts):
        ready(part)
        rows = rows_ref[...]
        gate_pre = jnp.dot(rows, gate_ref[part], preferred_element_type=jnp.float32)
        up_pre = jnp.dot(rows, up_ref[part], preferred_element_type=jnp.float32)
        gate_pre = jnp.minimum(gate_pre, clamp_limit)
        up_pre = jnp.clip(up_pre, -clamp_limit, clamp_limit)
        hidden_ref[:, part * tile : (part + 1) * tile] = (
            (up_pre + 1.0) * (gate_pre * jax.nn.sigmoid(alpha_gate * gate_pre))
        ).astype(jnp.bfloat16)
    for part in range(columns):
        ready(parts + part)
        result = jnp.dot(hidden_ref[...], down_ref[part], preferred_element_type=jnp.float32)
        start = 0
        for ref in out_refs:
            ref[:, part * column : (part + 1) * column] = result[
                start : start + ref.shape[0]
            ].astype(ref.dtype)
            start += ref.shape[0]


def expert_rows(rows, gain, weights, room):
    count, width = sum(block.shape[0] for block in rows), rows[0].shape[1]
    hidden = weights[0].shape[2]
    tile, column = math.gcd(hidden, 256), math.gcd(width, 512)
    parts, columns = hidden // tile, width // column
    held = pl.BlockSpec(memory_space=pltpu.VMEM)
    return pl.pallas_call(
        functools.partial(expert_kernel, len(rows)),
        in_specs=[pl.BlockSpec(memory_space=pl.ANY)] * 4 + [held] * len(rows),
        out_specs=[held] * len(rows),
        out_shape=block_shapes(count, width, len(rows)),
        scratch_shapes=[
            pltpu.VMEM((parts, width, tile), jnp.bfloat16),
            pltpu.VMEM((parts, width, tile), jnp.bfloat16),
            pltpu.VMEM((columns, hidden, column), jnp.bfloat16),
            pltpu.VMEM((count, hidden), jnp.bfloat16),
            pltpu.VMEM((count, width), jnp.float32),
            pltpu.VMEM((count, width), jnp.bfloat16),
            pltpu.VMEM(gain.shape, gain.dtype),
            pltpu.SemaphoreType.DMA((parts + columns + 1, 2)),
        ],
        compiler_params=pltpu.CompilerParams(vmem_limit_bytes=room),
        cost_estimate=pl.CostEstimate(
            flops=6 * count * width * hidden,
            bytes_accessed=2 * (3 * width * hidden + 2 * count * width),
            transcendentals=count * hidden,
        ),
    )(gain, *weights, *rows)


def hop_order(members):
    half = members // 2
    return [half | mask for mask in range(half)] + list(range(half - 1, 0, -1))


def hops(blocks, masks):
    members = len(blocks)
    arrived = {
        mask: lax.ppermute(blocks[mask], NEAR, [(i, i ^ mask) for i in range(members)])
        for mask in masks
    }
    return arrived


def in_order(first, arrived):
    return [first] + [arrived[mask] for mask in sorted(arrived)]


def exchange(rows, members):
    parts = rows.reshape(members, -1, rows.shape[1])
    return lax.all_to_all(parts, NEAR, split_axis=0, concat_axis=0, tiled=True).reshape(rows.shape)


def gated_input(gate_inner, conv_input):
    return (gate_inner.astype(jnp.float32) * conv_input.astype(jnp.float32)).astype(jnp.bfloat16)


def mixer(gate_outer, gate_inner, conv_input, previous, conv_taps, mixer_out_weight):
    rows_here = gate_inner.shape[0]
    product = gated_input(gate_inner, conv_input)
    extended = jnp.concatenate([previous, product], 0).astype(jnp.float32)
    convolved = jnp.zeros(product.shape, jnp.float32)
    for offset in range(conv_taps.shape[0]):
        convolved = convolved + conv_taps[offset][None, :] * extended[offset : offset + rows_here]
    gated_rows = (gate_outer.astype(jnp.float32) * convolved).astype(jnp.bfloat16)
    return jnp.dot(gated_rows, mixer_out_weight, preferred_element_type=jnp.float32).astype(
        jnp.bfloat16
    )


def shards(
    gate_outer,
    gate_inner,
    conv_input,
    conv_taps,
    mixer_out_weight,
    moe_tokens,
    norm_gain,
    expert_ids,
    route_weight,
    expert_gate,
    expert_up,
    expert_down,
):
    tokens_here, top_count = expert_ids.shape
    members = lax.axis_size(NEAR)
    capacity = 3 * tokens_here * top_count // (2 * lax.axis_size(EVERY))
    capacity = -(-capacity // 8) * 8
    slots = members * capacity
    masks = hop_order(members)
    gain = norm_gain[None, :]
    ids, route = expert_ids.T, route_weight.T
    weights = (expert_gate, expert_up, expert_down)

    far_tokens = swap_halves(moe_tokens)
    far_ids = swap_halves(ids)
    far_route = swap_halves(route)
    last = gate_inner.shape[0] - (conv_taps.shape[0] - 1)
    previous = from_behind(gated_input(gate_inner[last:], conv_input[last:]), EVERY, 1)
    slot, send = to_slots(ids, moe_tokens, slots, capacity, members, WIDE_VMEM)
    first_go, first_back = members * 7 // 16, members // 2
    received = hops(send, masks[:first_go])
    far_slot, far_send = to_slots(far_ids, far_tokens, slots, capacity, 1, SMALL_VMEM)
    far_received = exchange(far_send[0], members)
    received |= hops(send, masks[first_go:])
    received = in_order(send[0], received)
    far_out = expert_rows([far_received], gain, weights, EXPERT_VMEM)
    far_back = exchange(far_out[0], members)
    out = expert_rows(received, gain, weights, WIDE_VMEM)
    back = hops(out, masks[:first_back])
    far_total = from_slots(far_slot, far_route, [far_back], ())
    returned = swap_halves(far_total)
    back |= hops(out, masks[first_back:])
    mixed_out = mixer(
        gate_outer, gate_inner, conv_input, previous, conv_taps, mixer_out_weight
    )
    back = in_order(out[0], back)
    moe_out = from_slots(slot, route, back, (returned,))
    return (mixed_out, moe_out)


def solution(mesh):
    outer, inner = mesh.shape["ep"], mesh.shape["tp"]
    halves = 2 if outer % 2 == 0 else 1
    split = Mesh(mesh.devices.reshape(halves, outer // halves, inner), EVERY)
    rows = P(EVERY, None)
    weights = P(EVERY, None, None)
    in_specs = (rows, rows, rows, P(), P(), rows, P(), rows, rows, weights, weights, weights)
    return jax.shard_map(
        shards, mesh=split, in_specs=in_specs, out_specs=(rows, rows), check_vma=False
    )
```

```python
import functools
import math

import jax
import jax.numpy as jnp
from jax import lax
from jax.experimental import pallas as pl
from jax.experimental.pallas import tpu as pltpu
from jax.sharding import Mesh, PartitionSpec as P

epsilon = 1e-06
clamp_limit = 7.0
alpha_gate = 1.702
EVERY = ("half", "near", "tp")
NEAR = ("near", "tp")
SMALL_VMEM = 12 * 1024 * 1024
WIDE_VMEM = 58 * 1024 * 1024
EXPERT_VMEM = 50 * 1024 * 1024
AHEAD = 5


def from_behind(value, axis, by):
    length = lax.axis_size(axis)
    pairs = [(i, i + by) for i in range(length) if 0 <= i + by < length]
    return lax.ppermute(value, axis, pairs)


def swap_halves(value):
    halves, near = lax.axis_size("half"), lax.axis_size("near")
    shift = near // 2 if near % 2 == 0 and halves > 1 else 0
    pairs = [
        (h * near + n, (h + 1) % halves * near + (n + shift) % near)
        for h in range(halves)
        for n in range(near)
    ]
    return lax.ppermute(value, ("half", "near"), pairs)


def dispatch_kernel(capacity, masked, ids_ref, rows_ref, slot_ref, *send_refs):
    top_count, tokens = ids_ref.shape
    slots = sum(ref.shape[0] for ref in send_refs)
    experts_near = slots // capacity
    ids = ids_ref[...] - lax.axis_index("half") * experts_near
    member = lax.axis_index("near") * lax.axis_size("tp") + lax.axis_index("tp")
    experts = lax.broadcasted_iota(jnp.int32, (experts_near, tokens), 0)
    hits = [ids[k : k + 1, :] == experts for k in range(top_count)]
    named = functools.reduce(jnp.logical_or, hits)
    before = lax.broadcasted_iota(jnp.int32, (tokens, tokens), 0) < lax.broadcasted_iota(
        jnp.int32, (tokens, tokens), 1
    )
    rank = jnp.dot(
        named.astype(jnp.float32).astype(jnp.bfloat16),
        before.astype(jnp.float32).astype(jnp.bfloat16),
        preferred_element_type=jnp.float32,
    )
    slot_rows = lax.broadcasted_iota(jnp.int32, (slots, tokens), 0)
    here = None
    for k in range(top_count):
        own = jnp.sum(jnp.where(hits[k], rank, 0.0), axis=0, keepdims=True).astype(jnp.int32)
        choice = ids[k : k + 1, :]
        inside = (choice >= 0) & (choice < experts_near)
        block = choice ^ member if masked else choice
        slot = jnp.where(inside, block * capacity + own, slots)
        slot_ref[k : k + 1, :] = slot
        match = slot_rows == slot
        here = match if here is None else here | match
    laid = jnp.dot(
        here.astype(jnp.float32).astype(jnp.bfloat16),
        rows_ref[...],
        preferred_element_type=jnp.float32,
    )
    start = 0
    for ref in send_refs:
        ref[...] = laid[start : start + ref.shape[0]].astype(ref.dtype)
        start += ref.shape[0]


def block_shapes(slots, width, blocks):
    return [jax.ShapeDtypeStruct((slots // blocks, width), jnp.bfloat16)] * blocks


def to_slots(ids, rows, slots, capacity, blocks, room):
    top_count, tokens = ids.shape
    width = rows.shape[1]
    held = pl.BlockSpec(memory_space=pltpu.VMEM)
    slot, *send = pl.pallas_call(
        functools.partial(dispatch_kernel, capacity, blocks > 1),
        in_specs=[held, held],
        out_specs=[held] * (1 + blocks),
        out_shape=[jax.ShapeDtypeStruct((top_count, tokens), jnp.int32)]
        + block_shapes(slots, width, blocks),
        compiler_params=pltpu.CompilerParams(vmem_limit_bytes=room),
        cost_estimate=pl.CostEstimate(
            flops=2 * slots * tokens * width,
            bytes_accessed=2 * (slots + tokens) * width,
            transcendentals=0,
        ),
    )(ids, rows)
    return slot, send


def gather_blocks(refs, wide_ref):
    if len(refs) == 1:
        return refs[0][...]
    start = 0
    for ref in refs:
        wide_ref[start : start + ref.shape[0], :] = ref[...].astype(jnp.float32)
        start += ref.shape[0]
    return wide_ref[...].astype(jnp.bfloat16)


def combine_kernel(blocks, addends, slot_ref, weight_ref, *refs):
    back_refs, add_refs = refs[:blocks], refs[blocks : blocks + addends]
    out_ref, wide_ref = refs[blocks + addends :]
    slots = sum(ref.shape[0] for ref in back_refs)
    top_count, tokens = slot_ref.shape
    weights = weight_ref[...]
    mix = weights / jnp.sum(weights, axis=0, keepdims=True)
    slot_rows = lax.broadcasted_iota(jnp.int32, (slots, tokens), 0)
    share = jnp.zeros((slots, tokens), jnp.float32)
    for k in range(top_count):
        share = jnp.where(slot_rows == slot_ref[k : k + 1, :], mix[k : k + 1, :], share)
    high = share.astype(jnp.bfloat16)
    low = (share - high.astype(jnp.float32)).astype(jnp.bfloat16)
    back = gather_blocks(back_refs, wide_ref)
    over = (((0,), (0,)), ((), ()))
    total = lax.dot_general(high, back, over, preferred_element_type=jnp.float32)
    total = total + lax.dot_general(low, back, over, preferred_element_type=jnp.float32)
    for ref in add_refs:
        total = total + ref[...].astype(jnp.float32)
    out_ref[...] = total.astype(out_ref.dtype)


def from_slots(slot, weights, back, addends):
    slots, width = sum(block.shape[0] for block in back), back[0].shape[1]
    tokens = slot.shape[1]
    wide = (slots, width) if len(back) > 1 else (8, 128)
    return pl.pallas_call(
        functools.partial(combine_kernel, len(back), len(addends)),
        in_specs=[pl.BlockSpec(memory_space=pltpu.VMEM)] * (2 + len(back) + len(addends)),
        out_specs=pl.BlockSpec(memory_space=pltpu.VMEM),
        out_shape=jax.ShapeDtypeStruct((tokens, width), jnp.bfloat16),
        scratch_shapes=[pltpu.VMEM(wide, jnp.float32)],
        compiler_params=pltpu.CompilerParams(vmem_limit_bytes=SMALL_VMEM),
        cost_estimate=pl.CostEstimate(
            flops=4 * slots * tokens * width,
            bytes_accessed=2 * (slots + tokens) * width,
            transcendentals=0,
        ),
    )(slot, weights, *back, *addends)


def expert_kernel(blocks, gain, gate, up, down, *refs):
    in_refs, out_refs = refs[:blocks], refs[blocks : 2 * blocks]
    gate_ref, up_ref, down_ref, hidden_ref, wide_ref, rows_ref, gain_ref, sems = refs[
        2 * blocks : 2 * blocks + 8
    ]
    leaving = []
    parts, _, tile = gate_ref.shape
    columns, _, column = down_ref.shape
    work = []
    for part in range(parts):
        cut = pl.ds(part * tile, tile)
        work.append(((gate, gate_ref, part, cut), (up, up_ref, part, cut)))
    for part in range(columns):
        work.append(((down, down_ref, part, pl.ds(part * column, column)),))
    copies = [
        [
            pltpu.make_async_copy(source.at[0, :, cut], target.at[part], sems.at[step, at])
            for at, (source, target, part, cut) in enumerate(pieces)
        ]
        for step, pieces in enumerate(work)
    ]

    def ready(step):
        for copy in copies[step]:
            copy.wait()
        if step + AHEAD < len(copies):
            for copy in copies[step + AHEAD]:
                copy.start()

    scale_copy = pltpu.make_async_copy(gain, gain_ref, sems.at[len(copies), 0])
    scale_copy.start()
    for step in range(min(AHEAD, len(copies))):
        for copy in copies[step]:
            copy.start()
    height = in_refs[0].shape[0]
    for block, ref in enumerate(in_refs if blocks > 1 else ()):
        wide_ref[block * height : (block + 1) * height, :] = ref[...].astype(jnp.float32)
    scale_copy.wait()
    count = wide_ref.shape[0]
    band = math.gcd(count, 64)
    for top in range(0, count, band):
        source = wide_ref if blocks > 1 else in_refs[0]
        tokens = source[top : top + band, :].astype(jnp.float32)
        scale = lax.rsqrt(jnp.mean(tokens * tokens, axis=-1, keepdims=True) + epsilon)
        rows_ref[top : top + band, :] = (tokens * scale * gain_ref[...]).astype(jnp.bfloat16)
    for part in range(parts):
        ready(part)
        rows = rows_ref[...]
        gate_pre = jnp.dot(rows, gate_ref[part], preferred_element_type=jnp.float32)
        up_pre = jnp.dot(rows, up_ref[part], preferred_element_type=jnp.float32)
        gate_pre = jnp.minimum(gate_pre, clamp_limit)
        up_pre = jnp.clip(up_pre, -clamp_limit, clamp_limit)
        hidden_ref[:, part * tile : (part + 1) * tile] = (
            (up_pre + 1.0) * (gate_pre * jax.nn.sigmoid(alpha_gate * gate_pre))
        ).astype(jnp.bfloat16)
    for part in range(columns):
        ready(parts + part)
        result = jnp.dot(hidden_ref[...], down_ref[part], preferred_element_type=jnp.float32)
        cut = slice(part * column, (part + 1) * column)
        if blocks == 1:
            made_ref = refs[-1]
            made_ref[part] = result.astype(made_ref.dtype)
            leaving.append(
                pltpu.make_async_copy(
                    made_ref.at[part], out_refs[0].at[:, cut], sems.at[len(copies) + 1 + part, 0]
                )
            )
            leaving[-1].start()
            continue
        start = 0
        for ref in out_refs:
            ref[:, cut] = result[start : start + ref.shape[0]].astype(ref.dtype)
            start += ref.shape[0]
    for copy in leaving:
        copy.wait()


def expert_rows(rows, gain, weights, room):
    count, width = sum(block.shape[0] for block in rows), rows[0].shape[1]
    hidden = weights[0].shape[2]
    tile, column = math.gcd(hidden, 256), math.gcd(width, 512)
    parts, columns = hidden // tile, width // column
    held = pl.BlockSpec(memory_space=pltpu.VMEM)
    return pl.pallas_call(
        functools.partial(expert_kernel, len(rows)),
        in_specs=[pl.BlockSpec(memory_space=pl.ANY)] * 4 + [held] * len(rows),
        out_specs=[pl.BlockSpec(memory_space=pl.ANY) if len(rows) == 1 else held] * len(rows),
        out_shape=block_shapes(count, width, len(rows)),
        scratch_shapes=[
            pltpu.VMEM((parts, width, tile), jnp.bfloat16),
            pltpu.VMEM((parts, width, tile), jnp.bfloat16),
            pltpu.VMEM((columns, hidden, column), jnp.bfloat16),
            pltpu.VMEM((count, hidden), jnp.bfloat16),
            pltpu.VMEM((count, width), jnp.float32),
            pltpu.VMEM((count, width), jnp.bfloat16),
            pltpu.VMEM(gain.shape, gain.dtype),
            pltpu.SemaphoreType.DMA((parts + 2 * columns + 1, 2)),
            pltpu.VMEM((columns, count, column), jnp.bfloat16),
        ],
        compiler_params=pltpu.CompilerParams(vmem_limit_bytes=room),
        cost_estimate=pl.CostEstimate(
            flops=6 * count * width * hidden,
            bytes_accessed=2 * (3 * width * hidden + 2 * count * width),
            transcendentals=count * hidden,
        ),
    )(gain, *weights, *rows)


def hop_order(members):
    half = members // 2
    return [half | mask for mask in range(half)] + list(range(half - 1, 0, -1))


def hops(blocks, masks):
    members = len(blocks)
    arrived = {
        mask: lax.ppermute(blocks[mask], NEAR, [(i, i ^ mask) for i in range(members)])
        for mask in masks
    }
    return arrived


def in_order(first, arrived):
    return [first] + [arrived[mask] for mask in sorted(arrived)]


def exchange(rows, members):
    parts = rows.reshape(members, -1, rows.shape[1])
    return lax.all_to_all(parts, NEAR, split_axis=0, concat_axis=0, tiled=True).reshape(rows.shape)


def gated_input(gate_inner, conv_input):
    return (gate_inner.astype(jnp.float32) * conv_input.astype(jnp.float32)).astype(jnp.bfloat16)


def mixer(gate_outer, gate_inner, conv_input, previous, conv_taps, mixer_out_weight):
    rows_here = gate_inner.shape[0]
    product = gated_input(gate_inner, conv_input)
    extended = jnp.concatenate([previous, product], 0).astype(jnp.float32)
    convolved = jnp.zeros(product.shape, jnp.float32)
    for offset in range(conv_taps.shape[0]):
        convolved = convolved + conv_taps[offset][None, :] * extended[offset : offset + rows_here]
    gated_rows = (gate_outer.astype(jnp.float32) * convolved).astype(jnp.bfloat16)
    return jnp.dot(gated_rows, mixer_out_weight, preferred_element_type=jnp.float32).astype(
        jnp.bfloat16
    )


def shards(
    gate_outer,
    gate_inner,
    conv_input,
    conv_taps,
    mixer_out_weight,
    moe_tokens,
    norm_gain,
    expert_ids,
    route_weight,
    expert_gate,
    expert_up,
    expert_down,
):
    tokens_here, top_count = expert_ids.shape
    members = lax.axis_size(NEAR)
    capacity = 3 * tokens_here * top_count // (2 * lax.axis_size(EVERY))
    capacity = -(-capacity // 8) * 8
    slots = members * capacity
    masks = hop_order(members)
    gain = norm_gain[None, :]
    ids, route = expert_ids.T, route_weight.T
    weights = (expert_gate, expert_up, expert_down)

    far_tokens = swap_halves(moe_tokens)
    far_ids = swap_halves(ids)
    far_route = swap_halves(route)
    last = gate_inner.shape[0] - (conv_taps.shape[0] - 1)
    previous = from_behind(gated_input(gate_inner[last:], conv_input[last:]), EVERY, 1)
    slot, send = to_slots(ids, moe_tokens, slots, capacity, members, WIDE_VMEM)
    first_go, first_back = members * 7 // 16, members // 2
    received = hops(send, masks[:first_go])
    far_slot, far_send = to_slots(far_ids, far_tokens, slots, capacity, 1, SMALL_VMEM)
    far_received = exchange(far_send[0], members)
    received |= hops(send, masks[first_go:])
    received = in_order(send[0], received)
    far_out = expert_rows([far_received], gain, weights, EXPERT_VMEM)
    far_back = exchange(far_out[0], members)
    out = expert_rows(received, gain, weights, WIDE_VMEM)
    back = hops(out, masks[:first_back])
    far_total = from_slots(far_slot, far_route, [far_back], ())
    returned = swap_halves(far_total)
    back |= hops(out, masks[first_back:])
    mixed_out = mixer(
        gate_outer, gate_inner, conv_input, previous, conv_taps, mixer_out_weight
    )
    back = in_order(out[0], back)
    moe_out = from_slots(slot, route, back, (returned,))
    return (mixed_out, moe_out)


def solution(mesh):
    outer, inner = mesh.shape["ep"], mesh.shape["tp"]
    halves = 2 if outer % 2 == 0 else 1
    split = Mesh(mesh.devices.reshape(halves, outer // halves, inner), EVERY)
    rows = P(EVERY, None)
    weights = P(EVERY, None, None)
    in_specs = (rows, rows, rows, P(), P(), rows, P(), rows, rows, weights, weights, weights)
    return jax.shard_map(
        shards, mesh=split, in_specs=in_specs, out_specs=(rows, rows), check_vma=False
    )
```
